32 devices in a mesh: sp: 16 (over z, y, x), tp: 2 (over core).
Axes of the slice: x: 2, y: 2, z: 4, core: 2. Of those that a mesh axis runs over, the one named last changes fastest.
Arguments:
- hidden_in: bfloat16 [8192, 2048], P('sp'), may hold values from -64 to 64
- pre_gain: float32 [2048], replicated, may hold values from 0.1 to 1.9
- query_proj: bfloat16 [2048, 2048], P(None, 'tp'), may hold values from -2 to 2
- key_proj: bfloat16 [2048, 2048], P('sp', 'tp'), may hold values from -2 to 2
- value_proj: bfloat16 [2048, 2048], P('sp', 'tp'), may hold values from -0.125 to 0.125
- out_proj: bfloat16 [2048, 2048], P('tp'), may hold values from -0.125 to 0.125
- post_gain: float32 [2048], replicated, may hold values from 0.1 to 1.9
Outputs:
- layer_out: bfloat16 [8192, 2048], P(('sp', 'tp'))
- log_weight: float32 [32, 8192], P('tp', 'sp')
The draws below stay inside these ranges and needn't reach their ends.
All inputs are finite; a program needn't handle non-finite values.
Results may differ from the reference program's by a relative error of at most 0.018.
The reference program's roundings to bfloat16 on the way count: a program that leaves them out, or rounds other values in their place, can miss the bound.
Values may be sent and summed in bfloat16 or wider, within the bound.
A program may use at most 128 MiB of HBM per device.

```python
import jax
import jax.numpy as jnp
from jax import lax

D = 2048
HEADS = 32
HEAD_DIM = 64
SPAN = 128
TOKENS = 8192
N_TP = 2


def draw_hidden_in(key, part):
    noise_part = jax.random.normal(jax.random.fold_in(key, 3), (TOKENS, D), jnp.float32)
    return jnp.clip(noise_part, -64.0, 64.0).astype(jnp.bfloat16)


def shared_pair(key):
    fan_scale = D ** (-0.5)
    query_part = jax.random.normal(jax.random.fold_in(key, 22), (D, HEADS * HEAD_DIM), jnp.float32) * fan_scale
    key_part = jax.random.normal(jax.random.fold_in(key, 23), (D, HEADS * HEAD_DIM), jnp.float32) * fan_scale
    return (jnp.clip(query_part, -2.0, 2.0), jnp.clip(key_part, -2.0, 2.0))


def draw_query_proj(key, part):
    return shared_pair(key)[0].astype(jnp.bfloat16)


def draw_key_proj(key, part):
    return shared_pair(key)[1].astype(jnp.bfloat16)


def steps_of(key, dims, split, least, high):
    factor_of = 1.0
    for dim, parts in split:
        steps = jax.random.uniform(jax.random.fold_in(jax.random.fold_in(key, 6), dim), (parts,), jnp.float32, least / len(split), high / len(split))
        factor_of = factor_of * jnp.repeat(jnp.exp(steps), dims[dim] // parts).reshape((-1,) + (1,) * (len(dims) - 1 - dim))
    return factor_of


def noise(key, shape, deviation, most, shards=(), held_as=jnp.bfloat16):
    values = jax.random.normal(key, shape, jnp.float32) * deviation
    if len(shards) > 0:
        values = steps_of(key, shape, shards, -0.22, 0.18) * values
    return jnp.clip(values, min=-most, max=most).astype(held_as)


def setup_inputs(seed: int = 0) -> dict:
    splits = jax.random.split(jax.random.key(seed), 8)
    return {
        "hidden_in": draw_hidden_in(jax.random.fold_in(splits[7], 71), 0),
        "pre_gain": jnp.clip(1.0 + 0.18 * jax.random.normal(splits[1], (D,), jnp.float32), 0.1, 1.9),
        "query_proj": draw_query_proj(jax.random.fold_in(splits[7], 71), 0),
        "key_proj": draw_key_proj(jax.random.fold_in(splits[7], 71), 0),
        "value_proj": noise(splits[4], (D, HEADS * HEAD_DIM), D ** -0.5, 0.125, ((0, 16), (1, 2))),
        "out_proj": noise(splits[5], (HEADS * HEAD_DIM, D), (HEADS * HEAD_DIM) ** -0.5, 0.125, ((0, 2),)),
        "post_gain": jnp.clip(1.0 + 0.18 * jax.random.normal(splits[6], (D,), jnp.float32), 0.1, 1.9),
    }


EPS = 1e-06
ROPE_BASE = 10000.0
DILATIONS = (1, 4, 16)

def rotate(vectors, positions):
    half_dim = vectors.shape[-1] // 2
    frequency = ROPE_BASE ** (-(jnp.arange(half_dim, dtype=jnp.float32) * 2.0 / vectors.shape[-1]))
    angles = positions[:, None] * frequency[None, :]
    cos_part = jnp.cos(angles)[:, None, :]
    sin_part = jnp.sin(angles)[:, None, :]
    front_half = vectors[..., :half_dim]
    back_half = vectors[..., half_dim:]
    return jnp.concatenate([front_half * cos_part - back_half * sin_part, back_half * cos_part + front_half * sin_part], axis=-1)

def rms_scale(matrix, gain):
    return matrix * lax.rsqrt(lax.optimization_barrier(jnp.mean(matrix * matrix, axis=-1, keepdims=True)) + EPS) * gain

def residue_attention(queries, key_rows, values, dilation):
    seq_len, head_count, head_depth = queries.shape
    blocks = seq_len // (dilation * SPAN)
    block_shape = (blocks, SPAN, dilation, head_count, head_depth)
    query_blocks = queries.reshape(block_shape).astype(jnp.float32)
    key_blocks = key_rows.reshape(block_shape).astype(jnp.float32)
    value_blocks = values.reshape(block_shape).astype(jnp.float32)
    zero_block = jnp.zeros((1,) + block_shape[1:], jnp.float32)
    key_pairs = jnp.concatenate([jnp.concatenate([zero_block, key_blocks[:-1]], axis=0), key_blocks], axis=1)
    value_pairs = jnp.concatenate([jnp.concatenate([zero_block, value_blocks[:-1]], axis=0), value_blocks], axis=1)
    scores = jnp.einsum('bqrhe,bkrhe->brhqk', query_blocks, key_pairs) * head_depth ** (-0.5)
    query_idx = jnp.arange(SPAN, dtype=jnp.int32)[:, None]
    key_idx = jnp.arange(2 * SPAN, dtype=jnp.int32)[None, :]
    distance = query_idx + SPAN - key_idx
    in_band = (distance >= 0) & (distance <= SPAN)
    key_pos = (jnp.arange(blocks, dtype=jnp.int32)[:, None, None, None, None] * SPAN + jnp.arange(2 * SPAN, dtype=jnp.int32)[None, None, None, None, :] - SPAN) * dilation + jnp.arange(dilation, dtype=jnp.int32)[None, :, None, None, None]
    valid = in_band[None, None, None] & (key_pos >= 0)
    scores = jnp.where(valid, scores, -jnp.inf)
    row_max = lax.optimization_barrier(jnp.max(scores, axis=-1, keepdims=True))
    exp_scores = jnp.exp(scores - row_max)
    denominator = lax.optimization_barrier(jnp.sum(exp_scores, axis=-1, keepdims=True))
    levels = (row_max + jnp.log(denominator))[..., 0]
    shares = lax.optimization_barrier((exp_scores / denominator).astype(jnp.bfloat16))
    outcome = jnp.einsum('brhqk,bkrhe->bqrhe', shares.astype(jnp.float32), value_pairs)
    outcome = outcome.reshape(seq_len, head_count, head_depth)
    levels = levels.transpose(2, 0, 3, 1).reshape(head_count, seq_len)
    return (outcome, levels)

def blend(group_outs, group_levels):
    levels = jnp.stack(group_levels)
    row_max = lax.optimization_barrier(jnp.max(levels, axis=0))
    log_weight = row_max + jnp.log(lax.optimization_barrier(jnp.sum(jnp.exp(levels - row_max[None]), axis=0)))
    shares = jnp.exp(levels - log_weight[None])
    blended = lax.optimization_barrier(jnp.sum(shares.transpose(0, 2, 1)[..., None] * jnp.stack(group_outs), axis=0))
    return (blended, log_weight)

def reference(hidden_in, pre_gain, query_proj, key_proj, value_proj, out_proj, post_gain):
    normed = rms_scale(hidden_in.astype(jnp.float32), pre_gain).astype(jnp.bfloat16)
    positions = jnp.arange(TOKENS, dtype=jnp.int32).astype(jnp.float32)
    group_width = HEADS // N_TP * HEAD_DIM

    def split_cols(matrix):
        return matrix.reshape(D, N_TP, group_width).transpose(1, 0, 2)

    def one_group(summed, weights):
        w_query, w_key, w_value, w_out = weights
        queries = rotate(jnp.dot(normed, w_query, preferred_element_type=jnp.float32).reshape(TOKENS, -1, HEAD_DIM), positions).astype(jnp.bfloat16)
        key_rows = rotate(jnp.dot(normed, w_key, preferred_element_type=jnp.float32).reshape(TOKENS, -1, HEAD_DIM), positions).astype(jnp.bfloat16)
        values = jnp.dot(normed, w_value, preferred_element_type=jnp.float32).astype(jnp.bfloat16).reshape(TOKENS, -1, HEAD_DIM)
        group_outs = []
        group_levels = []
        for dilation in DILATIONS:
            outcome, levels = residue_attention(queries, key_rows, values, dilation)
            group_outs.append(outcome)
            group_levels.append(levels)
        blended, log_weight = blend(group_outs, group_levels)
        attended = blended.astype(jnp.bfloat16).reshape(TOKENS, group_width)
        partial_value = lax.optimization_barrier(jnp.dot(attended, w_out, preferred_element_type=jnp.float32).astype(jnp.bfloat16))
        return (summed + partial_value.astype(jnp.float32), log_weight)
    summed, log_weight = lax.scan(one_group, jnp.zeros((TOKENS, D), jnp.float32), (split_cols(query_proj), split_cols(key_proj), split_cols(value_proj), out_proj.reshape(N_TP, group_width, D)))
    layer_out = rms_scale(summed, post_gain).astype(jnp.bfloat16)
    return (layer_out, log_weight.reshape(HEADS, TOKENS))
```

```python
import functools

import jax
import jax.numpy as jnp
from jax import lax
from jax.experimental import pallas as pl
from jax.experimental.pallas import tpu as pltpu
from jax.sharding import PartitionSpec as P

HEAD_DIM = 64
SPAN = 128
EPS = 1e-06
ROPE_BASE = 10000.0
WIDE = 16
LANES = 128
MESH = pl.DeviceIdType.MESH
ANY = pl.BlockSpec(memory_space=pl.ANY)
NEG = -1e30


def greet(peers):
    barrier = pltpu.get_barrier_semaphore()
    for peer in peers:
        pl.semaphore_signal(barrier, inc=1, device_id=peer, device_id_type=MESH)
    pl.semaphore_wait(barrier, len(peers))


def remote(src, dst, send, recv, peer):
    return pltpu.make_async_remote_copy(
        src_ref=src, dst_ref=dst, send_sem=send, recv_sem=recv, device_id=peer, device_id_type=MESH
    )


def group_of(mesh, width):
    for size in (4, 2):
        if mesh.shape["sp"] % size == 0 and width % (size * LANES) == 0:
            return size
    return 1


def gather_kernel(n_sp, group, hid_ref, wk_ref, wv_ref, hid_out, wk_out, wv_out, hs, hr, fs, fr, ws, wr, local):
    s = lax.axis_index("sp")
    t = lax.axis_index("tp")
    rows = hid_ref.shape[0]
    half_rows = rows // 2
    depth, width = wk_ref.shape
    part = width // group
    c = lax.rem(s, group)
    base = s - c
    half = lax.rem(t, 2)
    sibling = (s, t + 1 - 2 * half)
    near = [base + lax.rem(c + k, group) for k in range(1, group)]
    far = [lax.rem(s + k, n_sp) for k in range(1, n_sp)]
    greet([(peer, t) for peer in far] + [sibling])
    mine = pl.ds(pl.multiple_of(half * half_rows, half_rows), half_rows)

    copies = []
    for k, peer in enumerate(near):
        copies.append(remote(hid_ref.at[mine], hid_out.at[c, mine], hs.at[k], hr.at[k], (peer, t)))
        copies[-1].start()
    weights = []
    for k, peer in enumerate(far):
        cols = pl.ds(pl.multiple_of(lax.rem(peer, group) * part, LANES), part)
        into = pl.ds(pl.multiple_of(s * depth, depth), depth)
        for j, (src, dst) in enumerate(((wk_ref, wk_out), (wv_ref, wv_out))):
            weights.append(remote(src.at[:, cols], dst.at[into], ws.at[2 * k + j], wr.at[2 * k + j], (peer, t)))
            weights[-1].start()
    own = remote(hid_ref, hid_out.at[c], hs.at[group - 1], hr.at[group - 1], sibling)
    own.start()
    cols = pl.ds(pl.multiple_of(c * part, LANES), part)
    into = pl.ds(pl.multiple_of(s * depth, depth), depth)
    kept = [
        pltpu.make_async_copy(wk_ref.at[:, cols], wk_out.at[into], local.at[0]),
        pltpu.make_async_copy(wv_ref.at[:, cols], wv_out.at[into], local.at[1]),
    ]
    for copy in kept:
        copy.start()
    forwards = []
    for k in range(1, group):
        copies[k - 1].wait_recv()
        slot = hid_out.at[lax.rem(c + group - k, group), mine]
        forwards.append(remote(slot, slot, fs.at[k - 1], fr.at[k - 1], sibling))
        forwards[-1].start()
    for copy in copies:
        copy.wait_send()
    for copy in forwards + weights + [own] + kept:
        copy.wait()


def gather(mesh, group, hidden, key_proj, value_proj):
    n_sp = mesh.shape["sp"]
    depth, width = key_proj.shape
    part = width // group
    dma = pltpu.SemaphoreType.DMA
    weight = jax.ShapeDtypeStruct((n_sp * depth, part), key_proj.dtype)
    return pl.pallas_call(
        functools.partial(gather_kernel, n_sp, group),
        out_shape=(jax.ShapeDtypeStruct((group,) + hidden.shape, hidden.dtype), weight, weight),
        in_specs=[ANY] * 3,
        out_specs=(ANY,) * 3,
        scratch_shapes=[
            dma((group,)), dma((group,)), dma((group,)), dma((group,)),
            dma((2 * n_sp,)), dma((2 * n_sp,)), dma((2,)),
        ],
        compiler_params=pltpu.CompilerParams(collective_id=0, has_side_effects=True),
        name="gather_blocks",
    )(hidden, key_proj, value_proj)


def project_kernel(part, hid_ref, gain_ref, wq_ref, wk_ref, wv_ref, cos_ref, sin_ref, nat_ref, res_ref, scr):
    x = hid_ref[...].astype(jnp.float32)
    normed = x * lax.rsqrt(jnp.mean(x * x, axis=-1, keepdims=True) + EPS) * gain_ref[...]
    normed = normed.astype(jnp.bfloat16)
    rows = x.shape[0]
    front = lax.rem(lax.broadcasted_iota(jnp.int32, (rows, LANES), 1), HEAD_DIM) < HEAD_DIM // 2
    for j, w_ref in enumerate((wq_ref, wk_ref, wv_ref)):
        out = jnp.dot(normed, w_ref[...], preferred_element_type=jnp.float32)
        for i in range(part // LANES):
            u = out[:, i * LANES:(i + 1) * LANES]
            if j < 2:
                swapped = jnp.where(
                    front,
                    pltpu.roll(u, LANES - HEAD_DIM // 2, 1),
                    pltpu.roll(u, HEAD_DIM // 2, 1),
                )
                u = u * cos_ref[...] + swapped * sin_ref[...]
            if j == 0:
                u = u * HEAD_DIM ** (-0.5)
            scr[j * (part // LANES) + i] = u
    for i in range(3 * part // LANES):
        cols = pl.ds(i * LANES, LANES)
        nat_ref[:, cols] = scr[i].astype(jnp.bfloat16)
        for r in range(WIDE):
            res_ref[r, :, cols] = scr[i, pl.ds(r, rows // WIDE, stride=WIDE), :].astype(jnp.bfloat16)


def project(hid, gain, wq, wk, wv, cos_part, sin_part):
    rows, depth = hid.shape
    part = wk.shape[1]
    block = 256
    whole = pl.BlockSpec((depth, part), lambda i: (0, 0))
    table = pl.BlockSpec((block, LANES), lambda i: (i, 0))
    return pl.pallas_call(
        functools.partial(project_kernel, part),
        grid=(rows // block,),
        out_shape=(
            jax.ShapeDtypeStruct((rows, 3 * part), jnp.bfloat16),
            jax.ShapeDtypeStruct((WIDE, rows // WIDE, 3 * part), jnp.bfloat16),
        ),
        in_specs=[
            pl.BlockSpec((block, depth), lambda i: (i, 0)),
            pl.BlockSpec((1, depth), lambda i: (0, 0)),
            whole, whole, whole, table, table,
        ],
        out_specs=(
            pl.BlockSpec((block, 3 * part), lambda i: (i, 0)),
            pl.BlockSpec((WIDE, block // WIDE, 3 * part), lambda i: (0, i, 0)),
        ),
        scratch_shapes=[pltpu.VMEM((3 * part // LANES, block, LANES), jnp.float32)],
        compiler_params=pltpu.CompilerParams(vmem_limit_bytes=50 * 1024 * 1024),
        cost_estimate=pl.CostEstimate(flops=6 * rows * depth * part, bytes_accessed=2 * rows * depth, transcendentals=0),
        name="project_rows",
    )(hid, gain, wq, wk, wv, cos_part, sin_part)


def halo_kernel(n_sp, group, behind, part, nat_ref, res_ref, res_out, nat_out, send, recv):
    s = lax.axis_index("sp")
    t = lax.axis_index("tp")
    after = [lax.rem(s + b * group, n_sp) for b in range(1, behind + 1)]
    before = [lax.rem(s + n_sp - b * group, n_sp) for b in range(1, behind + 1)]
    greet([(peer, t) for peer in after + before])
    cols = pl.ds(part, 2 * part)
    last = pl.ds(nat_ref.shape[0] - SPAN, SPAN)
    copies = [remote(nat_ref.at[last, cols], nat_out, send.at[0], recv.at[0], (after[0], t))]
    for b in range(1, behind + 1):
        copies.append(
            remote(res_ref.at[:, :, cols], res_out.at[behind - b], send.at[b], recv.at[b], (after[b - 1], t))
        )
    for copy in copies:
        copy.start()
    for copy in copies:
        copy.wait()


def halo(mesh, group, behind, nat, res):
    part = nat.shape[1] // 3
    dma = pltpu.SemaphoreType.DMA
    return pl.pallas_call(
        functools.partial(halo_kernel, mesh.shape["sp"], group, behind, part),
        out_shape=(
            jax.ShapeDtypeStruct((behind, WIDE, res.shape[1], 2 * part), jnp.bfloat16),
            jax.ShapeDtypeStruct((SPAN, 2 * part), jnp.bfloat16),
        ),
        in_specs=[ANY] * 2,
        out_specs=(ANY,) * 2,
        scratch_shapes=[dma((behind + 1,)), dma((behind + 1,))],
        compiler_params=pltpu.CompilerParams(collective_id=1, has_side_effects=True),
        name="send_earlier",
    )(nat, res)


def attend_kernel(
    group, behind,
    qn, kn, vn, qr, kr, vr, hkr, hvr, hkn, hvn,
    out_ref, lw_ref,
    kx, vx, kw, vw, acc4, m4, l4, acc16, m16, l16, b1, b4, b16,
):
    rows = qn.shape[0]
    steps = rows // WIDE
    block = min(SPAN, steps)
    g = lax.axis_index("sp") // group
    f32 = jnp.float32
    for b in range(behind):
        kx[:, b * steps:(b + 1) * steps, :] = hkr[b]
        vx[:, b * steps:(b + 1) * steps, :] = hvr[b]
    kx[:, SPAN:, :] = kr[...]
    vx[:, SPAN:, :] = vr[...]
    kw[:SPAN, :] = hkn[...]
    vw[:SPAN, :] = hvn[...]
    kw[SPAN:, :] = kn[...]
    vw[SPAN:, :] = vn[...]

    def put_bias(ref, near, count, first_of):
        shape = ref.shape[1:]
        a = lax.broadcasted_iota(jnp.int32, shape, 0)
        b = lax.broadcasted_iota(jnp.int32, shape, 1)
        distance, place = near(a, b)
        band = (distance >= 0) & (distance <= SPAN)
        ref[0] = jnp.where(band & (place + first_of >= 0), 0.0, NEG).astype(f32)
        ref[1] = jnp.where(band, 0.0, NEG).astype(f32)

    def plain(a, b):
        return a + SPAN - b, b - SPAN

    def woven(a, b):
        return 4 * (a % 32 + 32 - b % 64) + a // 32 - b // 64, b % 64 - 32

    put_bias(b1, plain, 0, g * rows)
    put_bias(b16, plain, 0, g * steps)
    put_bias(b4, woven, 0, g * steps)

    def tile(q, k, v, bias):
        count = q.shape[0]
        low = lax.broadcasted_iota(jnp.int32, (count, LANES), 1) < HEAD_DIM
        low_q = low.astype(f32).astype(jnp.bfloat16)
        both = jnp.concatenate([q * low_q, q * (1 - low_q)], axis=0)
        s = lax.dot_general(both, k, (((1,), (1,)), ((), ())), preferred_element_type=f32)
        s = s + jnp.concatenate([bias, bias], axis=0)
        m = jnp.max(s, axis=-1, keepdims=True)
        p = jnp.exp(s - m).astype(jnp.bfloat16)
        o = jnp.dot(p, jnp.concatenate([v, jnp.ones_like(v)], axis=1), preferred_element_type=f32)
        wide_m = jnp.broadcast_to(m, (2 * count, LANES))
        return (
            jnp.where(low, o[:count, :LANES], o[count:, :LANES]),
            jnp.where(low, wide_m[:count], wide_m[count:]),
            jnp.where(low, o[:count, LANES:], o[count:, LANES:]),
        )

    blocks16 = steps // block

    def step16(idx, _):
        r = idx // blocks16
        i = idx % blocks16
        at = pl.multiple_of(i * block, block)
        keys = pl.ds(at, block + SPAN)
        got = tile(qr[r, pl.ds(at, block), :], kx[r, keys, :], vx[r, keys, :], b16[jnp.minimum(i, 1)])
        for ref, value in zip((acc16, m16, l16), got):
            ref[pl.ds(r + WIDE * at, block, stride=WIDE), :] = value
        return 0

    lax.fori_loop(0, WIDE * blocks16, step16, 0, unroll=2)
    blocks4 = steps // 32

    def step4(idx, _):
        r = idx // blocks4
        i = idx % blocks4
        at = pl.multiple_of(i * 32, 32)
        keys = pl.ds(pl.multiple_of(at + SPAN - 32, 32), 64)
        got = tile(
            jnp.concatenate([qr[r + 4 * j, pl.ds(at, 32), :] for j in range(4)], axis=0),
            jnp.concatenate([kx[r + 4 * j, keys, :] for j in range(4)], axis=0),
            jnp.concatenate([vx[r + 4 * j, keys, :] for j in range(4)], axis=0),
            b4[jnp.minimum(i, 1)],
        )
        for ref, value in zip((acc4, m4, l4), got):
            for j in range(4):
                ref[pl.ds(r + 4 * j + WIDE * at, 32, stride=WIDE), :] = value[j * 32:(j + 1) * 32]
        return 0

    lax.fori_loop(0, 4 * blocks4, step4, 0, unroll=2)

    def step1(i, _):
        at = pl.multiple_of(i * SPAN, SPAN)
        here = pl.ds(at, SPAN)
        keys = pl.ds(at, 2 * SPAN)
        acc, m, l = tile(qn[here, :], kw[keys, :], vw[keys, :], b1[jnp.minimum(i, 1)])
        top = jnp.maximum(m, jnp.maximum(m4[here, :], m16[here, :]))
        e1, e4, e16 = (jnp.exp(x - top) for x in (m, m4[here, :], m16[here, :]))
        total = l * e1 + l4[here, :] * e4 + l16[here, :] * e16
        mixed = acc * e1 + acc4[here, :] * e4 + acc16[here, :] * e16
        out_ref[here, :] = (mixed / total).astype(out_ref.dtype)
        turned = jnp.transpose(top + jnp.log(total))
        lw_ref[0, 0:1, here] = turned[0:1]
        lw_ref[0, 1:2, here] = turned[HEAD_DIM:HEAD_DIM + 1]
        return 0

    lax.fori_loop(0, rows // SPAN, step1, 0, unroll=2)


def attend(mesh, group, behind, nat, res, res_halo, nat_halo):
    rows, part3 = nat.shape
    part = part3 // 3
    pairs = part // LANES
    steps = rows // WIDE
    block = min(SPAN, steps)

    def nat_spec(count, off):
        return pl.BlockSpec((count, LANES), lambda p: (0, p + off))

    def res_spec(off):
        return pl.BlockSpec((WIDE, steps, LANES), lambda p: (0, 0, p + off))

    def halo_spec(off):
        return pl.BlockSpec((behind, WIDE, steps, LANES), lambda p: (0, 0, 0, p + off))

    f32 = jnp.float32
    state = pltpu.VMEM((rows, LANES), f32)
    return pl.pallas_call(
        functools.partial(attend_kernel, group, behind),
        grid=(pairs,),
        out_shape=(
            jax.ShapeDtypeStruct((rows, part), jnp.bfloat16),
            jax.ShapeDtypeStruct((pairs, 2, rows), f32),
        ),
        in_specs=[
            nat_spec(rows, 0), nat_spec(rows, pairs), nat_spec(rows, 2 * pairs),
            res_spec(0), res_spec(pairs), res_spec(2 * pairs),
            halo_spec(0), halo_spec(pairs),
            nat_spec(SPAN, 0), nat_spec(SPAN, pairs),
        ],
        out_specs=(
            pl.BlockSpec((rows, LANES), lambda p: (0, p)),
            pl.BlockSpec((1, 2, rows), lambda p: (p, 0, 0)),
        ),
        scratch_shapes=[
            pltpu.VMEM((WIDE, SPAN + steps, LANES), jnp.bfloat16),
            pltpu.VMEM((WIDE, SPAN + steps, LANES), jnp.bfloat16),
            pltpu.VMEM((SPAN + rows, LANES), jnp.bfloat16),
            pltpu.VMEM((SPAN + rows, LANES), jnp.bfloat16),
            state, state, state, state, state, state,
            pltpu.VMEM((2, SPAN, 2 * SPAN), f32),
            pltpu.VMEM((2, SPAN, 2 * SPAN), f32),
            pltpu.VMEM((2, block, block + SPAN), f32),
        ],
        compiler_params=pltpu.CompilerParams(vmem_limit_bytes=56 * 1024 * 1024),
        cost_estimate=pl.CostEstimate(flops=6 * rows * 512 * part, bytes_accessed=8 * rows * part, transcendentals=0),
        name="attend_windows",
    )(nat, nat, nat, res, res, res, res_halo, res_halo, nat_halo, nat_halo)


def return_kernel(group, rows, att_ref, lw_ref, att_out, lw_out, send, recv, local):
    s = lax.axis_index("sp")
    t = lax.axis_index("tp")
    part = att_ref.shape[1]
    c = lax.rem(s, group)
    base = s - c
    peers = [lax.rem(c + k, group) for k in range(1, group)]
    if group > 1:
        greet([(base + peer, t) for peer in peers])
    cols = pl.ds(pl.multiple_of(c * part, LANES), part)

    def pieces(peer):
        span = pl.ds(pl.multiple_of(peer * rows, rows), rows)
        return ((att_ref.at[span], att_out.at[:, cols]), (lw_ref.at[:, :, span], lw_out.at[c]))

    copies = []
    for k, peer in enumerate(peers):
        for j, (src, dst) in enumerate(pieces(peer)):
            copies.append(remote(src, dst, send.at[2 * k + j], recv.at[2 * k + j], (base + peer, t)))
    for j, (src, dst) in enumerate(pieces(c)):
        copies.append(pltpu.make_async_copy(src, dst, local.at[j]))
    for copy in copies:
        copy.start()
    for copy in copies:
        copy.wait()


def give_back(mesh, group, att, lw):
    rows = att.shape[0] // group
    part = att.shape[1]
    pairs = part // LANES
    dma = pltpu.SemaphoreType.DMA
    return pl.pallas_call(
        functools.partial(return_kernel, group, rows),
        out_shape=(
            jax.ShapeDtypeStruct((rows, part * group), att.dtype),
            jax.ShapeDtypeStruct((group, pairs, 2, rows), lw.dtype),
        ),
        in_specs=[ANY] * 2,
        out_specs=(ANY,) * 2,
        scratch_shapes=[dma((2 * group,)), dma((2 * group,)), dma((2,))],
        compiler_params=pltpu.CompilerParams(
            collective_id=2 if group > 1 else None, has_side_effects=True
        ),
        name="give_back",
    )(att, lw)


def swap_kernel(n_tp, part_ref, out_ref, send, recv):
    s = lax.axis_index("sp")
    t = lax.axis_index("tp")
    peers = [lax.rem(t + k, n_tp) for k in range(1, n_tp)]
    greet([(s, peer) for peer in peers])
    copies = [
        remote(part_ref.at[peer], out_ref.at[k], send.at[k], recv.at[k], (s, peer))
        for k, peer in enumerate(peers)
    ]
    for copy in copies:
        copy.start()
    for copy in copies:
        copy.wait()


def swap(mesh, partial):
    n_tp = mesh.shape["tp"]
    dma = pltpu.SemaphoreType.DMA
    return pl.pallas_call(
        functools.partial(swap_kernel, n_tp),
        out_shape=jax.ShapeDtypeStruct((n_tp - 1,) + partial.shape[1:], partial.dtype),
        in_specs=[ANY],
        out_specs=ANY,
        scratch_shapes=[dma((n_tp,)), dma((n_tp,))],
        compiler_params=pltpu.CompilerParams(collective_id=3, has_side_effects=True),
        name="swap_partials",
    )(partial)


def tables(rows, offset):
    half = HEAD_DIM // 2
    frequency = ROPE_BASE ** (-(jnp.arange(half, dtype=jnp.float32) * 2.0 / HEAD_DIM))
    positions = (offset + jnp.arange(rows, dtype=jnp.int32)).astype(jnp.float32)
    angles = positions[:, None] * frequency[None, :]
    cos_part = jnp.cos(angles)
    sin_part = jnp.sin(angles)
    return (
        jnp.concatenate([cos_part] * 4, axis=1),
        jnp.concatenate([-sin_part, sin_part] * 2, axis=1),
    )


def body(mesh, hidden_in, pre_gain, query_proj, key_proj, value_proj, out_proj, post_gain):
    rows, depth = hidden_in.shape
    width = query_proj.shape[1]
    n_tp = mesh.shape["tp"]
    group = group_of(mesh, width)
    part = width // group
    s = lax.axis_index("sp")
    t = lax.axis_index("tp")
    c = lax.rem(s, group)
    all_rows = rows * group
    behind = -(-(WIDE * SPAN) // all_rows)
    hid, wk, wv = gather(mesh, group, hidden_in, key_proj, value_proj)
    wq = lax.dynamic_slice_in_dim(query_proj, c * part, part, axis=1)
    cos_part, sin_part = tables(all_rows, (s - c) * rows)
    nat, res = project(
        hid.reshape(all_rows, depth), pre_gain[None, :], wq, wk, wv, cos_part, sin_part
    )
    res_halo, nat_halo = halo(mesh, group, behind, nat, res)
    att, lw = attend(mesh, group, behind, nat, res, res_halo, nat_halo)
    attended, log_weight = give_back(mesh, group, att, lw)
    partial = jnp.dot(attended, out_proj, preferred_element_type=jnp.float32).astype(jnp.bfloat16)
    partial = partial.reshape(n_tp, rows // n_tp, depth)
    others = swap(mesh, partial)
    own = lax.dynamic_index_in_dim(partial, t, 0, keepdims=False)
    summed = own.astype(jnp.float32) + jnp.sum(others.astype(jnp.float32), axis=0)
    scale = lax.rsqrt(jnp.mean(summed * summed, axis=-1, keepdims=True) + EPS)
    layer_out = (summed * scale * post_gain).astype(jnp.bfloat16)
    return (layer_out, log_weight.reshape(width // HEAD_DIM, rows))


def solution(mesh):
    placed = (P("sp", None), P(), P(None, "tp"), P("sp", "tp"), P("sp", "tp"), P("tp", None), P())
    return jax.shard_map(
        functools.partial(body, mesh),
        mesh=mesh,
        in_specs=placed,
        out_specs=(P(("sp", "tp"), None), P("tp", "sp")),
        check_vma=False,
    )
```

```python
import functools

import jax
import jax.numpy as jnp
from jax import lax
from jax.experimental import pallas as pl
from jax.experimental.pallas import tpu as pltpu
from jax.sharding import PartitionSpec as P

HEAD_DIM = 64
SPAN = 128
EPS = 1e-06
ROPE_BASE = 10000.0
WIDE = 16
LANES = 128
MESH = pl.DeviceIdType.MESH
ANY = pl.BlockSpec(memory_space=pl.ANY)
NEG = -1e30


def greet(peers):
    barrier = pltpu.get_barrier_semaphore()
    for peer in peers:
        pl.semaphore_signal(barrier, inc=1, device_id=peer, device_id_type=MESH)
    pl.semaphore_wait(barrier, len(peers))


def remote(src, dst, send, recv, peer):
    return pltpu.make_async_remote_copy(
        src_ref=src, dst_ref=dst, send_sem=send, recv_sem=recv, device_id=peer, device_id_type=MESH
    )


def group_of(mesh, width):
    for size in (4, 2):
        if mesh.shape["sp"] % size == 0 and width % (size * LANES) == 0:
            return size
    return 1


def gather_kernel(n_sp, group, hid_ref, wk_ref, wv_ref, hid_out, wk_out, wv_out, hs, hr, fs, fr, ws, wr, local):
    s = lax.axis_index("sp")
    t = lax.axis_index("tp")
    rows = hid_ref.shape[0]
    half_rows = rows // 2
    depth, width = wk_ref.shape
    part = width // group
    c = lax.rem(s, group)
    base = s - c
    half = lax.rem(t, 2)
    sibling = (s, t + 1 - 2 * half)
    near = [base + lax.rem(c + k, group) for k in range(1, group)]
    far = [lax.rem(s + k * group, n_sp) for k in range(1, n_sp // group)]
    greet([(peer, t) for peer in near + far] + [sibling])
    mine = pl.ds(pl.multiple_of(half * half_rows, half_rows), half_rows)

    pairs = ((wk_ref, wk_out), (wv_ref, wv_out))
    into = pl.ds(pl.multiple_of(s * depth, depth), depth)
    cols = pl.ds(pl.multiple_of(c * part, LANES), part)
    kept = [
        pltpu.make_async_copy(src.at[:, cols], dst.at[into], local.at[j])
        for j, (src, dst) in enumerate(pairs)
    ]
    for copy in kept:
        copy.start()
    weights = []
    for k, peer in enumerate(near):
        cols = pl.ds(pl.multiple_of((peer - base) * part, LANES), part)
        for j, (src, dst) in enumerate(pairs):
            weights.append(remote(src.at[:, cols], dst.at[into], ws.at[2 * k + j], wr.at[2 * k + j], (peer, t)))
            weights[-1].start()
    copies = []
    for k, peer in enumerate(near):
        copies.append(remote(hid_ref.at[mine], hid_out.at[c, mine], hs.at[k], hr.at[k], (peer, t)))
        copies[-1].start()
    own = remote(hid_ref, hid_out.at[c], hs.at[group - 1], hr.at[group - 1], sibling)
    own.start()
    for copy in kept + weights:
        copy.wait()
    slot = pl.ds(pl.multiple_of(base * depth, depth), group * depth)
    passed = []
    for k, peer in enumerate(far):
        for j, (_, dst) in enumerate(pairs):
            at = 2 * (group - 1 + k) + j
            passed.append(remote(dst.at[slot], dst.at[slot], ws.at[at], wr.at[at], (peer, t)))
            passed[-1].start()
    forwards = []
    for k in range(1, group):
        copies[k - 1].wait_recv()
        slot = hid_out.at[lax.rem(c + group - k, group), mine]
        forwards.append(remote(slot, slot, fs.at[k - 1], fr.at[k - 1], sibling))
        forwards[-1].start()
    for copy in copies:
        copy.wait_send()
    for copy in forwards + passed + [own]:
        copy.wait()


def gather(mesh, group, hidden, key_proj, value_proj):
    n_sp = mesh.shape["sp"]
    depth, width = key_proj.shape
    part = width // group
    dma = pltpu.SemaphoreType.DMA
    weight = jax.ShapeDtypeStruct((n_sp * depth, part), key_proj.dtype)
    return pl.pallas_call(
        functools.partial(gather_kernel, n_sp, group),
        out_shape=(jax.ShapeDtypeStruct((group,) + hidden.shape, hidden.dtype), weight, weight),
        in_specs=[ANY] * 3,
        out_specs=(ANY,) * 3,
        scratch_shapes=[
            dma((group,)), dma((group,)), dma((group,)), dma((group,)),
            dma((2 * n_sp,)), dma((2 * n_sp,)), dma((2,)),
        ],
        compiler_params=pltpu.CompilerParams(collective_id=0, has_side_effects=True),
        name="gather_blocks",
    )(hidden, key_proj, value_proj)


def project_kernel(part, hid_ref, gain_ref, wq_ref, wk_ref, wv_ref, cos_ref, sin_ref, nat_ref, res_ref, scr):
    x = hid_ref[...].astype(jnp.float32)
    normed = x * lax.rsqrt(jnp.mean(x * x, axis=-1, keepdims=True) + EPS) * gain_ref[...]
    normed = normed.astype(jnp.bfloat16)
    rows = x.shape[0]
    front = lax.rem(lax.broadcasted_iota(jnp.int32, (rows, LANES), 1), HEAD_DIM) < HEAD_DIM // 2
    for j, w_ref in enumerate((wq_ref, wk_ref, wv_ref)):
        out = jnp.dot(normed, w_ref[...], preferred_element_type=jnp.float32)
        for i in range(part // LANES):
            u = out[:, i * LANES:(i + 1) * LANES]
            if j < 2:
                swapped = jnp.where(
                    front,
                    pltpu.roll(u, LANES - HEAD_DIM // 2, 1),
                    pltpu.roll(u, HEAD_DIM // 2, 1),
                )
                u = u * cos_ref[...] + swapped * sin_ref[...]
            if j == 0:
                u = u * HEAD_DIM ** (-0.5)
            scr[j * (part // LANES) + i] = u
    for i in range(3 * part // LANES):
        cols = pl.ds(i * LANES, LANES)
        nat_ref[:, cols] = scr[i].astype(jnp.bfloat16)
        for r in range(WIDE):
            res_ref[r, :, cols] = scr[i, pl.ds(r, rows // WIDE, stride=WIDE), :].astype(jnp.bfloat16)


def project(hid, gain, wq, wk, wv, cos_part, sin_part):
    rows, depth = hid.shape
    part = wk.shape[1]
    block = 256
    whole = pl.BlockSpec((depth, part), lambda i: (0, 0))
    table = pl.BlockSpec((block, LANES), lambda i: (i, 0))
    return pl.pallas_call(
        functools.partial(project_kernel, part),
        grid=(rows // block,),
        out_shape=(
            jax.ShapeDtypeStruct((rows, 3 * part), jnp.bfloat16),
            jax.ShapeDtypeStruct((WIDE, rows // WIDE, 3 * part), jnp.bfloat16),
        ),
        in_specs=[
            pl.BlockSpec((block, depth), lambda i: (i, 0)),
            pl.BlockSpec((1, depth), lambda i: (0, 0)),
            whole, whole, whole, table, table,
        ],
        out_specs=(
            pl.BlockSpec((block, 3 * part), lambda i: (i, 0)),
            pl.BlockSpec((WIDE, block // WIDE, 3 * part), lambda i: (0, i, 0)),
        ),
        scratch_shapes=[pltpu.VMEM((3 * part // LANES, block, LANES), jnp.float32)],
        compiler_params=pltpu.CompilerParams(vmem_limit_bytes=50 * 1024 * 1024),
        cost_estimate=pl.CostEstimate(flops=6 * rows * depth * part, bytes_accessed=2 * rows * depth, transcendentals=0),
        name="project_rows",
    )(hid, gain, wq, wk, wv, cos_part, sin_part)


def halo_kernel(n_sp, group, behind, part, nat_ref, res_ref, res_out, nat_out, send, recv):
    s = lax.axis_index("sp")
    t = lax.axis_index("tp")
    after = [lax.rem(s + b * group, n_sp) for b in range(1, behind + 1)]
    before = [lax.rem(s + n_sp - b * group, n_sp) for b in range(1, behind + 1)]
    greet([(peer, t) for peer in after + before])
    cols = pl.ds(part, 2 * part)
    last = pl.ds(nat_ref.shape[0] - SPAN, SPAN)
    copies = [remote(nat_ref.at[last, cols], nat_out, send.at[0], recv.at[0], (after[0], t))]
    for b in range(1, behind + 1):
        copies.append(
            remote(res_ref.at[:, :, cols], res_out.at[behind - b], send.at[b], recv.at[b], (after[b - 1], t))
        )
    for copy in copies:
        copy.start()
    for copy in copies:
        copy.wait()


def halo(mesh, group, behind, nat, res):
    part = nat.shape[1] // 3
    dma = pltpu.SemaphoreType.DMA
    return pl.pallas_call(
        functools.partial(halo_kernel, mesh.shape["sp"], group, behind, part),
        out_shape=(
            jax.ShapeDtypeStruct((behind, WIDE, res.shape[1], 2 * part), jnp.bfloat16),
            jax.ShapeDtypeStruct((SPAN, 2 * part), jnp.bfloat16),
        ),
        in_specs=[ANY] * 2,
        out_specs=(ANY,) * 2,
        scratch_shapes=[dma((behind + 1,)), dma((behind + 1,))],
        compiler_params=pltpu.CompilerParams(collective_id=1, has_side_effects=True),
        name="send_earlier",
    )(nat, res)


def attend_kernel(
    group, behind,
    qn, kn, vn, qr, kr, vr, hkr, hvr, hkn, hvn,
    out_ref, lw_ref,
    kx, vx, kw, vw, acc4, m4, l4, acc16, m16, l16, b1, b4, b16,
):
    rows = qn.shape[0]
    steps = rows // WIDE
    block = min(SPAN, steps)
    g = lax.axis_index("sp") // group
    f32 = jnp.float32
    for b in range(behind):
        kx[:, b * steps:(b + 1) * steps, :] = hkr[b]
        vx[:, b * steps:(b + 1) * steps, :] = hvr[b]
    kx[:, SPAN:, :] = kr[...]
    vx[:, SPAN:, :] = vr[...]
    kw[:SPAN, :] = hkn[...]
    vw[:SPAN, :] = hvn[...]
    kw[SPAN:, :] = kn[...]
    vw[SPAN:, :] = vn[...]

    def put_bias(ref, near, count, first_of):
        shape = ref.shape[1:]
        a = lax.broadcasted_iota(jnp.int32, shape, 0)
        b = lax.broadcasted_iota(jnp.int32, shape, 1)
        distance, place = near(a, b)
        band = (distance >= 0) & (distance <= SPAN)
        ref[0] = jnp.where(band & (place + first_of >= 0), 0.0, NEG).astype(f32)
        ref[1] = jnp.where(band, 0.0, NEG).astype(f32)

    def plain(a, b):
        return a + SPAN - b, b - SPAN

    def woven(a, b):
        return 4 * (a % 32 + 32 - b % 64) + a // 32 - b // 64, b % 64 - 32

    put_bias(b1, plain, 0, g * rows)
    put_bias(b16, plain, 0, g * steps)
    put_bias(b4, woven, 0, g * steps)

    def tile(q, k, v, bias):
        count = q.shape[0]
        low = lax.broadcasted_iota(jnp.int32, (count, LANES), 1) < HEAD_DIM
        low_q = low.astype(f32).astype(jnp.bfloat16)
        both = jnp.concatenate([q * low_q, q * (1 - low_q)], axis=0)
        s = lax.dot_general(both, k, (((1,), (1,)), ((), ())), preferred_element_type=f32)
        s = s + jnp.concatenate([bias, bias], axis=0)
        m = jnp.max(s, axis=-1, keepdims=True)
        p = jnp.exp(s - m).astype(jnp.bfloat16)
        o = jnp.dot(p, jnp.concatenate([v, jnp.ones_like(v)], axis=1), preferred_element_type=f32)
        wide_m = jnp.broadcast_to(m, (2 * count, LANES))
        return (
            jnp.where(low, o[:count, :LANES], o[count:, :LANES]),
            jnp.where(low, wide_m[:count], wide_m[count:]),
            jnp.where(low, o[:count, LANES:], o[count:, LANES:]),
        )

    blocks16 = steps // block

    def step16(idx, _):
        r = idx // blocks16
        i = idx % blocks16
        at = pl.multiple_of(i * block, block)
        keys = pl.ds(at, block + SPAN)
        got = tile(qr[r, pl.ds(at, block), :], kx[r, keys, :], vx[r, keys, :], b16[jnp.minimum(i, 1)])
        for ref, value in zip((acc16, m16, l16), got):
            ref[pl.ds(r + WIDE * at, block, stride=WIDE), :] = value
        return 0

    lax.fori_loop(0, WIDE * blocks16, step16, 0, unroll=2)
    blocks4 = steps // 32

    def step4(idx, _):
        r = idx // blocks4
        i = idx % blocks4
        at = pl.multiple_of(i * 32, 32)
        keys = pl.ds(pl.multiple_of(at + SPAN - 32, 32), 64)
        got = tile(
            jnp.concatenate([qr[r + 4 * j, pl.ds(at, 32), :] for j in range(4)], axis=0),
            jnp.concatenate([kx[r + 4 * j, keys, :] for j in range(4)], axis=0),
            jnp.concatenate([vx[r + 4 * j, keys, :] for j in range(4)], axis=0),
            b4[jnp.minimum(i, 1)],
        )
        for ref, value in zip((acc4, m4, l4), got):
            for j in range(4):
                ref[pl.ds(r + 4 * j + WIDE * at, 32, stride=WIDE), :] = value[j * 32:(j + 1) * 32]
        return 0

    lax.fori_loop(0, 4 * blocks4, step4, 0, unroll=2)

    def step1(i, _):
        at = pl.multiple_of(i * SPAN, SPAN)
        here = pl.ds(at, SPAN)
        keys = pl.ds(at, 2 * SPAN)
        acc, m, l = tile(qn[here, :], kw[keys, :], vw[keys, :], b1[jnp.minimum(i, 1)])
        top = jnp.maximum(m, jnp.maximum(m4[here, :], m16[here, :]))
        e1, e4, e16 = (jnp.exp(x - top) for x in (m, m4[here, :], m16[here, :]))
        total = l * e1 + l4[here, :] * e4 + l16[here, :] * e16
        mixed = acc * e1 + acc4[here, :] * e4 + acc16[here, :] * e16
        out_ref[here, :] = (mixed / total).astype(out_ref.dtype)
        turned = jnp.transpose(top + jnp.log(total))
        lw_ref[0, 0:1, here] = turned[0:1]
        lw_ref[0, 1:2, here] = turned[HEAD_DIM:HEAD_DIM + 1]
        return 0

    lax.fori_loop(0, rows // SPAN, step1, 0, unroll=2)


def attend(mesh, group, behind, nat, res, res_halo, nat_halo):
    rows, part3 = nat.shape
    part = part3 // 3
    pairs = part // LANES
    steps = rows // WIDE
    block = min(SPAN, steps)

    def nat_spec(count, off):
        return pl.BlockSpec((count, LANES), lambda p: (0, p + off))

    def res_spec(off):
        return pl.BlockSpec((WIDE, steps, LANES), lambda p: (0, 0, p + off))

    def halo_spec(off):
        return pl.BlockSpec((behind, WIDE, steps, LANES), lambda p: (0, 0, 0, p + off))

    f32 = jnp.float32
    state = pltpu.VMEM((rows, LANES), f32)
    return pl.pallas_call(
        functools.partial(attend_kernel, group, behind),
        grid=(pairs,),
        out_shape=(
            jax.ShapeDtypeStruct((rows, part), jnp.bfloat16),
            jax.ShapeDtypeStruct((pairs, 2, rows), f32),
        ),
        in_specs=[
            nat_spec(rows, 0), nat_spec(rows, pairs), nat_spec(rows, 2 * pairs),
            res_spec(0), res_spec(pairs), res_spec(2 * pairs),
            halo_spec(0), halo_spec(pairs),
            nat_spec(SPAN, 0), nat_spec(SPAN, pairs),
        ],
        out_specs=(
            pl.BlockSpec((rows, LANES), lambda p: (0, p)),
            pl.BlockSpec((1, 2, rows), lambda p: (p, 0, 0)),
        ),
        scratch_shapes=[
            pltpu.VMEM((WIDE, SPAN + steps, LANES), jnp.bfloat16),
            pltpu.VMEM((WIDE, SPAN + steps, LANES), jnp.bfloat16),
            pltpu.VMEM((SPAN + rows, LANES), jnp.bfloat16),
            pltpu.VMEM((SPAN + rows, LANES), jnp.bfloat16),
            state, state, state, state, state, state,
            pltpu.VMEM((2, SPAN, 2 * SPAN), f32),
            pltpu.VMEM((2, SPAN, 2 * SPAN), f32),
            pltpu.VMEM((2, block, block + SPAN), f32),
        ],
        compiler_params=pltpu.CompilerParams(vmem_limit_bytes=56 * 1024 * 1024),
        cost_estimate=pl.CostEstimate(flops=6 * rows * 512 * part, bytes_accessed=8 * rows * part, transcendentals=0),
        name="attend_windows",
    )(nat, nat, nat, res, res, res, res_halo, res_halo, nat_halo, nat_halo)


def return_kernel(group, rows, att_ref, lw_ref, att_out, lw_out, send, recv, local):
    s = lax.axis_index("sp")
    t = lax.axis_index("tp")
    part = att_ref.shape[1]
    c = lax.rem(s, group)
    base = s - c
    peers = [lax.rem(c + k, group) for k in range(1, group)]
    if group > 1:
        greet([(base + peer, t) for peer in peers])
    cols = pl.ds(pl.multiple_of(c * part, LANES), part)

    def pieces(peer):
        span = pl.ds(pl.multiple_of(peer * rows, rows), rows)
        return ((att_ref.at[span], att_out.at[:, cols]), (lw_ref.at[:, :, span], lw_out.at[c]))

    copies = []
    for k, peer in enumerate(peers):
        for j, (src, dst) in enumerate(pieces(peer)):
            copies.append(remote(src, dst, send.at[2 * k + j], recv.at[2 * k + j], (base + peer, t)))
    for j, (src, dst) in enumerate(pieces(c)):
        copies.append(pltpu.make_async_copy(src, dst, local.at[j]))
    for copy in copies:
        copy.start()
    for copy in copies:
        copy.wait()


def give_back(mesh, group, att, lw):
    rows = att.shape[0] // group
    part = att.shape[1]
    pairs = part // LANES
    dma = pltpu.SemaphoreType.DMA
    return pl.pallas_call(
        functools.partial(return_kernel, group, rows),
        out_shape=(
            jax.ShapeDtypeStruct((rows, part * group), att.dtype),
            jax.ShapeDtypeStruct((group, pairs, 2, rows), lw.dtype),
        ),
        in_specs=[ANY] * 2,
        out_specs=(ANY,) * 2,
        scratch_shapes=[dma((2 * group,)), dma((2 * group,)), dma((2,))],
        compiler_params=pltpu.CompilerParams(
            collective_id=2 if group > 1 else None, has_side_effects=True
        ),
        name="give_back",
    )(att, lw)


def swap_kernel(n_tp, part_ref, out_ref, send, recv):
    s = lax.axis_index("sp")
    t = lax.axis_index("tp")
    peers = [lax.rem(t + k, n_tp) for k in range(1, n_tp)]
    greet([(s, peer) for peer in peers])
    copies = [
        remote(part_ref.at[peer], out_ref.at[k], send.at[k], recv.at[k], (s, peer))
        for k, peer in enumerate(peers)
    ]
    for copy in copies:
        copy.start()
    for copy in copies:
        copy.wait()


def swap(mesh, partial):
    n_tp = mesh.shape["tp"]
    dma = pltpu.SemaphoreType.DMA
    return pl.pallas_call(
        functools.partial(swap_kernel, n_tp),
        out_shape=jax.ShapeDtypeStruct((n_tp - 1,) + partial.shape[1:], partial.dtype),
        in_specs=[ANY],
        out_specs=ANY,
        scratch_shapes=[dma((n_tp,)), dma((n_tp,))],
        compiler_params=pltpu.CompilerParams(collective_id=3, has_side_effects=True),
        name="swap_partials",
    )(partial)


def tables(rows, offset):
    half = HEAD_DIM // 2
    frequency = ROPE_BASE ** (-(jnp.arange(half, dtype=jnp.float32) * 2.0 / HEAD_DIM))
    positions = (offset + jnp.arange(rows, dtype=jnp.int32)).astype(jnp.float32)
    angles = positions[:, None] * frequency[None, :]
    cos_part = jnp.cos(angles)
    sin_part = jnp.sin(angles)
    return (
        jnp.concatenate([cos_part] * 4, axis=1),
        jnp.concatenate([-sin_part, sin_part] * 2, axis=1),
    )


def body(mesh, hidden_in, pre_gain, query_proj, key_proj, value_proj, out_proj, post_gain):
    rows, depth = hidden_in.shape
    width = query_proj.shape[1]
    n_tp = mesh.shape["tp"]
    group = group_of(mesh, width)
    part = width // group
    s = lax.axis_index("sp")
    t = lax.axis_index("tp")
    c = lax.rem(s, group)
    all_rows = rows * group
    behind = -(-(WIDE * SPAN) // all_rows)
    hid, wk, wv = gather(mesh, group, hidden_in, key_proj, value_proj)
    wq = lax.dynamic_slice_in_dim(query_proj, c * part, part, axis=1)
    cos_part, sin_part = tables(all_rows, (s - c) * rows)
    nat, res = project(
        hid.reshape(all_rows, depth), pre_gain[None, :], wq, wk, wv, cos_part, sin_part
    )
    res_halo, nat_halo = halo(mesh, group, behind, nat, res)
    att, lw = attend(mesh, group, behind, nat, res, res_halo, nat_halo)
    attended, log_weight = give_back(mesh, group, att, lw)
    partial = jnp.dot(attended, out_proj, preferred_element_type=jnp.float32).astype(jnp.bfloat16)
    partial = partial.reshape(n_tp, rows // n_tp, depth)
    others = swap(mesh, partial)
    own = lax.dynamic_index_in_dim(partial, t, 0, keepdims=False)
    summed = own.astype(jnp.float32) + jnp.sum(others.astype(jnp.float32), axis=0)
    scale = lax.rsqrt(jnp.mean(summed * summed, axis=-1, keepdims=True) + EPS)
    layer_out = (summed * scale * post_gain).astype(jnp.bfloat16)
    return (layer_out, log_weight.reshape(width // HEAD_DIM, rows))


def solution(mesh):
    placed = (P("sp", None), P(), P(None, "tp"), P("sp", "tp"), P("sp", "tp"), P("tp", None), P())
    return jax.shard_map(
        functools.partial(body, mesh),
        mesh=mesh,
        in_specs=placed,
        out_specs=(P(("sp", "tp"), None), P("tp", "sp")),
        check_vma=False,
    )
```

```python
import functools

import jax
import jax.numpy as jnp
from jax import lax
from jax.experimental import pallas as pl
from jax.experimental.pallas import tpu as pltpu
from jax.sharding import PartitionSpec as P

HEAD_DIM = 64
SPAN = 128
EPS = 1e-06
ROPE_BASE = 10000.0
WIDE = 16
LANES = 128
MESH = pl.DeviceIdType.MESH
ANY = pl.BlockSpec(memory_space=pl.ANY)
NEG = -1e30


def greet(peers):
    barrier = pltpu.get_barrier_semaphore()
    for peer in peers:
        pl.semaphore_signal(barrier, inc=1, device_id=peer, device_id_type=MESH)
    pl.semaphore_wait(barrier, len(peers))


def remote(src, dst, send, recv, peer):
    return pltpu.make_async_remote_copy(
        src_ref=src, dst_ref=dst, send_sem=send, recv_sem=recv, device_id=peer, device_id_type=MESH
    )


def group_of(mesh, width):
    for size in (4, 2):
        if mesh.shape["sp"] % size == 0 and width % (size * LANES) == 0:
            return size
    return 1


def gather_kernel(n_sp, group, hid_ref, wk_ref, wv_ref, hid_out, wk_out, wv_out, hs, hr, fs, fr, ws, wr, local):
    s = lax.axis_index("sp")
    t = lax.axis_index("tp")
    rows = hid_ref.shape[0]
    half_rows = rows // 2
    depth, width = wk_ref.shape
    part = width // group
    c = lax.rem(s, group)
    base = s - c
    half = lax.rem(t, 2)
    sibling = (s, t + 1 - 2 * half)
    near = [base + lax.rem(c + k, group) for k in range(1, group)]
    far = [lax.rem(s + k * group, n_sp) for k in range(1, n_sp // group)]
    greet([(peer, t) for peer in near + far] + [sibling])
    mine = pl.ds(pl.multiple_of(half * half_rows, half_rows), half_rows)

    pairs = ((wk_ref, wk_out), (wv_ref, wv_out))
    into = pl.ds(pl.multiple_of(s * depth, depth), depth)
    cols = pl.ds(pl.multiple_of(c * part, LANES), part)
    kept = [
        pltpu.make_async_copy(src.at[:, cols], dst.at[into], local.at[j])
        for j, (src, dst) in enumerate(pairs)
    ]
    for copy in kept:
        copy.start()
    weights = []
    for k, peer in enumerate(near):
        cols = pl.ds(pl.multiple_of((peer - base) * part, LANES), part)
        for j, (src, dst) in enumerate(pairs):
            weights.append(remote(src.at[:, cols], dst.at[into], ws.at[2 * k + j], wr.at[2 * k + j], (peer, t)))
            weights[-1].start()
    copies = []
    for k, peer in enumerate(near):
        copies.append(remote(hid_ref.at[mine], hid_out.at[c, mine], hs.at[k], hr.at[k], (peer, t)))
        copies[-1].start()
    own = remote(hid_ref, hid_out.at[c], hs.at[group - 1], hr.at[group - 1], sibling)
    own.start()
    for copy in kept + weights:
        copy.wait()
    slot = pl.ds(pl.multiple_of(base * depth, depth), group * depth)
    passed = []
    for k, peer in enumerate(far):
        for j, (_, dst) in enumerate(pairs):
            at = 2 * (group - 1 + k) + j
            passed.append(remote(dst.at[slot], dst.at[slot], ws.at[at], wr.at[at], (peer, t)))
            passed[-1].start()
    forwards = []
    for k in range(1, group):
        copies[k - 1].wait_recv()
        slot = hid_out.at[lax.rem(c + group - k, group), mine]
        forwards.append(remote(slot, slot, fs.at[k - 1], fr.at[k - 1], sibling))
        forwards[-1].start()
    for copy in copies:
        copy.wait_send()
    for copy in forwards + passed + [own]:
        copy.wait()


def gather(mesh, group, hidden, key_proj, value_proj):
    n_sp = mesh.shape["sp"]
    depth, width = key_proj.shape
    part = width // group
    dma = pltpu.SemaphoreType.DMA
    weight = jax.ShapeDtypeStruct((n_sp * depth, part), key_proj.dtype)
    return pl.pallas_call(
        functools.partial(gather_kernel, n_sp, group),
        out_shape=(jax.ShapeDtypeStruct((group,) + hidden.shape, hidden.dtype), weight, weight),
        in_specs=[ANY] * 3,
        out_specs=(ANY,) * 3,
        scratch_shapes=[
            dma((group,)), dma((group,)), dma((group,)), dma((group,)),
            dma((2 * n_sp,)), dma((2 * n_sp,)), dma((2,)),
        ],
        compiler_params=pltpu.CompilerParams(collective_id=0, has_side_effects=True),
        name="gather_blocks",
    )(hidden, key_proj, value_proj)


def project_kernel(part, hid_ref, gain_ref, wq_ref, wk_ref, wv_ref, cos_ref, sin_ref, nat_ref, res_ref, scr):
    x = hid_ref[...].astype(jnp.float32)
    normed = x * lax.rsqrt(jnp.mean(x * x, axis=-1, keepdims=True) + EPS) * gain_ref[...]
    normed = normed.astype(jnp.bfloat16)
    rows = x.shape[0]
    front = lax.rem(lax.broadcasted_iota(jnp.int32, (rows, LANES), 1), HEAD_DIM) < HEAD_DIM // 2
    for j, w_ref in enumerate((wq_ref, wk_ref, wv_ref)):
        out = jnp.dot(normed, w_ref[...], preferred_element_type=jnp.float32)
        for i in range(part // LANES):
            u = out[:, i * LANES:(i + 1) * LANES]
            if j < 2:
                swapped = jnp.where(
                    front,
                    pltpu.roll(u, LANES - HEAD_DIM // 2, 1),
                    pltpu.roll(u, HEAD_DIM // 2, 1),
                )
                u = u * cos_ref[...] + swapped * sin_ref[...]
            if j == 0:
                u = u * HEAD_DIM ** (-0.5)
            scr[j * (part // LANES) + i] = u
    for i in range(3 * part // LANES):
        cols = pl.ds(i * LANES, LANES)
        nat_ref[:, cols] = scr[i].astype(jnp.bfloat16)
        for r in range(WIDE):
            res_ref[r, :, cols] = scr[i, pl.ds(r, rows // WIDE, stride=WIDE), :].astype(jnp.bfloat16)


def project(hid, gain, wq, wk, wv, cos_part, sin_part):
    rows, depth = hid.shape
    part = wk.shape[1]
    block = 256
    whole = pl.BlockSpec((depth, part), lambda i: (0, 0))
    table = pl.BlockSpec((block, LANES), lambda i: (i, 0))
    return pl.pallas_call(
        functools.partial(project_kernel, part),
        grid=(rows // block,),
        out_shape=(
            jax.ShapeDtypeStruct((rows, 3 * part), jnp.bfloat16),
            jax.ShapeDtypeStruct((WIDE, rows // WIDE, 3 * part), jnp.bfloat16),
        ),
        in_specs=[
            pl.BlockSpec((block, depth), lambda i: (i, 0)),
            pl.BlockSpec((1, depth), lambda i: (0, 0)),
            whole, whole, whole, table, table,
        ],
        out_specs=(
            pl.BlockSpec((block, 3 * part), lambda i: (i, 0)),
            pl.BlockSpec((WIDE, block // WIDE, 3 * part), lambda i: (0, i, 0)),
        ),
        scratch_shapes=[pltpu.VMEM((3 * part // LANES, block, LANES), jnp.float32)],
        compiler_params=pltpu.CompilerParams(vmem_limit_bytes=50 * 1024 * 1024),
        cost_estimate=pl.CostEstimate(flops=6 * rows * depth * part, bytes_accessed=2 * rows * depth, transcendentals=0),
        name="project_rows",
    )(hid, gain, wq, wk, wv, cos_part, sin_part)


def attend_kernel(
    n_sp, group, behind, pairs,
    nat_ref, res_ref, qn, kn, vn, qr, kr, vr,
    out_ref, lw_ref,
    kx_all, vx_all, kw_all, vw_all, acc1, m1, l1, acc4, m4, l4, acc16, m16, l16, b1, b4, b16, send, recv,
):
    rows = qn.shape[0]
    steps = rows // WIDE
    block = min(SPAN, steps)
    g = lax.axis_index("sp") // group
    f32 = jnp.float32
    s = lax.axis_index("sp")
    t = lax.axis_index("tp")
    p = pl.program_id(0)
    after = [lax.rem(s + b * group, n_sp) for b in range(1, behind + 1)]
    before = [lax.rem(s + n_sp - b * group, n_sp) for b in range(1, behind + 1)]
    last = pl.ds(rows - SPAN, SPAN)

    def early(pair):
        copies = []
        for j, (ref, first) in enumerate(((kw_all, pairs), (vw_all, 2 * pairs))):
            cols = pl.ds(pl.multiple_of((first + pair) * LANES, LANES), LANES)
            copies.append(remote(
                nat_ref.at[last, cols], ref.at[pair, pl.ds(0, SPAN)], send.at[pair, j], recv.at[pair, j], (after[0], t)
            ))
        return copies

    def late(pair):
        copies = []
        for j, (ref, first) in enumerate(((kx_all, pairs), (vx_all, 2 * pairs))):
            cols = pl.ds(pl.multiple_of((first + pair) * LANES, LANES), LANES)
            for b in range(1, behind + 1):
                at = 2 * b + j
                copies.append(remote(
                    res_ref.at[:, :, cols],
                    ref.at[pair, :, pl.ds((behind - b) * steps, steps)],
                    send.at[pair, at], recv.at[pair, at], (after[b - 1], t),
                ))
        return copies

    @pl.when(p == 0)
    def _():
        greet([(peer, t) for peer in after + before])
        for pair in range(pairs):
            for copy in early(pair):
                copy.start()
        for pair in range(pairs):
            for copy in late(pair):
                copy.start()

    kx, vx, kw, vw = (ref.at[p] for ref in (kx_all, vx_all, kw_all, vw_all))
    kx[:, SPAN:, :] = kr[...]
    vx[:, SPAN:, :] = vr[...]
    kw[SPAN:, :] = kn[...]
    vw[SPAN:, :] = vn[...]

    def put_bias(ref, near, count, first_of):
        shape = ref.shape[1:]
        a = lax.broadcasted_iota(jnp.int32, shape, 0)
        b = lax.broadcasted_iota(jnp.int32, shape, 1)
        distance, place = near(a, b)
        band = (distance >= 0) & (distance <= SPAN)
        ref[0] = jnp.where(band & (place + first_of >= 0), 0.0, NEG).astype(f32)
        ref[1] = jnp.where(band, 0.0, NEG).astype(f32)

    def plain(a, b):
        return a + SPAN - b, b - SPAN

    def woven(a, b):
        return 4 * (a % 32 + 32 - b % 64) + a // 32 - b // 64, b % 64 - 32

    put_bias(b1, plain, 0, g * rows)
    put_bias(b16, plain, 0, g * steps)
    put_bias(b4, woven, 0, g * steps)

    def tile(q, k, v, bias):
        count = q.shape[0]
        low = lax.broadcasted_iota(jnp.int32, (count, LANES), 1) < HEAD_DIM
        low_q = low.astype(f32).astype(jnp.bfloat16)
        both = jnp.concatenate([q * low_q, q * (1 - low_q)], axis=0)
        s = lax.dot_general(both, k, (((1,), (1,)), ((), ())), preferred_element_type=f32)
        s = s + jnp.concatenate([bias, bias], axis=0)
        m = jnp.max(s, axis=-1, keepdims=True)
        p = jnp.exp(s - m).astype(jnp.bfloat16)
        o = jnp.dot(p, jnp.concatenate([v, jnp.ones_like(v)], axis=1), preferred_element_type=f32)
        wide_m = jnp.broadcast_to(m, (2 * count, LANES))
        return (
            jnp.where(low, o[:count, :LANES], o[count:, :LANES]),
            jnp.where(low, wide_m[:count], wide_m[count:]),
            jnp.where(low, o[:count, LANES:], o[count:, LANES:]),
        )

    blocks16 = steps // block

    def step16(idx, _):
        r = idx // blocks16
        i = idx % blocks16
        at = pl.multiple_of(i * block, block)
        keys = pl.ds(at, block + SPAN)
        got = tile(qr[r, pl.ds(at, block), :], kx[r, keys, :], vx[r, keys, :], b16[jnp.minimum(i, 1)])
        for ref, value in zip((acc16, m16, l16), got):
            ref[pl.ds(r + WIDE * at, block, stride=WIDE), :] = value
        return 0

    blocks4 = steps // 32

    def step4(r, i):
        at = pl.multiple_of(i * 32, 32) if not isinstance(i, int) else i * 32
        keys = pl.ds(pl.multiple_of(at + SPAN - 32, 32) if not isinstance(i, int) else at + SPAN - 32, 64)
        got = tile(
            jnp.concatenate([qr[r + 4 * j, pl.ds(at, 32), :] for j in range(4)], axis=0),
            jnp.concatenate([kx[r + 4 * j, keys, :] for j in range(4)], axis=0),
            jnp.concatenate([vx[r + 4 * j, keys, :] for j in range(4)], axis=0),
            b4[0 if isinstance(i, int) else 1],
        )
        for ref, value in zip((acc4, m4, l4), got):
            for j in range(4):
                ref[pl.ds(r + 4 * j + WIDE * at, 32, stride=WIDE), :] = value[j * 32:(j + 1) * 32]
        return 0


    def step1(i, _):
        at = pl.multiple_of(i * SPAN, SPAN)
        here = pl.ds(at, SPAN)
        keys = pl.ds(at, 2 * SPAN)
        got = tile(qn[here, :], kw[keys, :], vw[keys, :], b1[jnp.minimum(i, 1)])
        for ref, value in zip((acc1, m1, l1), got):
            ref[here, :] = value
        return 0

    def merge(i, _):
        here = pl.ds(pl.multiple_of(i * SPAN, SPAN), SPAN)
        tops = (m1[here, :], m4[here, :], m16[here, :])
        top = jnp.maximum(tops[0], jnp.maximum(tops[1], tops[2]))
        e1, e4, e16 = (jnp.exp(x - top) for x in tops)
        total = l1[here, :] * e1 + l4[here, :] * e4 + l16[here, :] * e16
        mixed = acc1[here, :] * e1 + acc4[here, :] * e4 + acc16[here, :] * e16
        out_ref[here, :] = (mixed / total).astype(out_ref.dtype)
        turned = jnp.transpose(top + jnp.log(total))
        lw_ref[0, 0:1, here] = turned[0:1]
        lw_ref[0, 1:2, here] = turned[HEAD_DIM:HEAD_DIM + 1]
        return 0

    if blocks4 > 1:
        lax.fori_loop(
            0, 4 * (blocks4 - 1),
            lambda idx, _: step4(idx // (blocks4 - 1), idx % (blocks4 - 1) + 1), 0, unroll=2,
        )
    for copy in early(p):
        copy.wait()
    lax.fori_loop(0, rows // SPAN, step1, 0, unroll=2)
    for copy in late(p):
        copy.wait()
    lax.fori_loop(0, 4, lambda r, _: step4(r, 0), 0, unroll=2)
    lax.fori_loop(0, WIDE * blocks16, step16, 0, unroll=2)
    lax.fori_loop(0, rows // SPAN, merge, 0, unroll=2)


def attend(mesh, group, behind, nat, res):
    rows, part3 = nat.shape
    part = part3 // 3
    pairs = part // LANES
    steps = rows // WIDE
    block = min(SPAN, steps)

    def nat_spec(count, off):
        return pl.BlockSpec((count, LANES), lambda p: (0, p + off))

    def res_spec(off):
        return pl.BlockSpec((WIDE, steps, LANES), lambda p: (0, 0, p + off))

    f32 = jnp.float32
    state = pltpu.VMEM((rows, LANES), f32)
    return pl.pallas_call(
        functools.partial(attend_kernel, mesh.shape["sp"], group, behind, pairs),
        grid=(pairs,),
        out_shape=(
            jax.ShapeDtypeStruct((rows, part), jnp.bfloat16),
            jax.ShapeDtypeStruct((pairs, 2, rows), f32),
        ),
        in_specs=[
            ANY, ANY,
            nat_spec(rows, 0), nat_spec(rows, pairs), nat_spec(rows, 2 * pairs),
            res_spec(0), res_spec(pairs), res_spec(2 * pairs),
        ],
        out_specs=(
            pl.BlockSpec((rows, LANES), lambda p: (0, p)),
            pl.BlockSpec((1, 2, rows), lambda p: (p, 0, 0)),
        ),
        scratch_shapes=[
            pltpu.VMEM((pairs, WIDE, SPAN + steps, LANES), jnp.bfloat16),
            pltpu.VMEM((pairs, WIDE, SPAN + steps, LANES), jnp.bfloat16),
            pltpu.VMEM((pairs, SPAN + rows, LANES), jnp.bfloat16),
            pltpu.VMEM((pairs, SPAN + rows, LANES), jnp.bfloat16),
            state, state, state, state, state, state, state, state, state,
            pltpu.VMEM((2, SPAN, 2 * SPAN), f32),
            pltpu.VMEM((2, SPAN, 2 * SPAN), f32),
            pltpu.VMEM((2, block, block + SPAN), f32),
            pltpu.SemaphoreType.DMA((pairs, 2 * behind + 2)),
            pltpu.SemaphoreType.DMA((pairs, 2 * behind + 2)),
        ],
        compiler_params=pltpu.CompilerParams(
            vmem_limit_bytes=56 * 1024 * 1024, collective_id=1, has_side_effects=True
        ),
        cost_estimate=pl.CostEstimate(flops=6 * rows * 512 * part, bytes_accessed=8 * rows * part, transcendentals=0),
        name="attend_windows",
    )(nat, res, nat, nat, nat, res, res, res)


def return_kernel(group, rows, att_ref, lw_ref, att_out, lw_out, send, recv, local):
    s = lax.axis_index("sp")
    t = lax.axis_index("tp")
    part = att_ref.shape[1]
    c = lax.rem(s, group)
    base = s - c
    peers = [lax.rem(c + k, group) for k in range(1, group)]
    if group > 1:
        greet([(base + peer, t) for peer in peers])
    cols = pl.ds(pl.multiple_of(c * part, LANES), part)

    def pieces(peer):
        span = pl.ds(pl.multiple_of(peer * rows, rows), rows)
        return ((att_ref.at[span], att_out.at[:, cols]), (lw_ref.at[:, :, span], lw_out.at[c]))

    copies = []
    for k, peer in enumerate(peers):
        for j, (src, dst) in enumerate(pieces(peer)):
            copies.append(remote(src, dst, send.at[2 * k + j], recv.at[2 * k + j], (base + peer, t)))
    for j, (src, dst) in enumerate(pieces(c)):
        copies.append(pltpu.make_async_copy(src, dst, local.at[j]))
    for copy in copies:
        copy.start()
    for copy in copies:
        copy.wait()


def give_back(mesh, group, att, lw):
    rows = att.shape[0] // group
    part = att.shape[1]
    pairs = part // LANES
    dma = pltpu.SemaphoreType.DMA
    return pl.pallas_call(
        functools.partial(return_kernel, group, rows),
        out_shape=(
            jax.ShapeDtypeStruct((rows, part * group), att.dtype),
            jax.ShapeDtypeStruct((group, pairs, 2, rows), lw.dtype),
        ),
        in_specs=[ANY] * 2,
        out_specs=(ANY,) * 2,
        scratch_shapes=[dma((2 * group,)), dma((2 * group,)), dma((2,))],
        compiler_params=pltpu.CompilerParams(
            collective_id=2 if group > 1 else None, has_side_effects=True
        ),
        name="give_back",
    )(att, lw)


def swap_kernel(n_tp, part_ref, out_ref, send, recv):
    s = lax.axis_index("sp")
    t = lax.axis_index("tp")
    peers = [lax.rem(t + k, n_tp) for k in range(1, n_tp)]
    greet([(s, peer) for peer in peers])
    copies = [
        remote(part_ref.at[peer], out_ref.at[k], send.at[k], recv.at[k], (s, peer))
        for k, peer in enumerate(peers)
    ]
    for copy in copies:
        copy.start()
    for copy in copies:
        copy.wait()


def swap(mesh, partial):
    n_tp = mesh.shape["tp"]
    dma = pltpu.SemaphoreType.DMA
    return pl.pallas_call(
        functools.partial(swap_kernel, n_tp),
        out_shape=jax.ShapeDtypeStruct((n_tp - 1,) + partial.shape[1:], partial.dtype),
        in_specs=[ANY],
        out_specs=ANY,
        scratch_shapes=[dma((n_tp,)), dma((n_tp,))],
        compiler_params=pltpu.CompilerParams(collective_id=3, has_side_effects=True),
        name="swap_partials",
    )(partial)


def tables(rows, offset):
    half = HEAD_DIM // 2
    frequency = ROPE_BASE ** (-(jnp.arange(half, dtype=jnp.float32) * 2.0 / HEAD_DIM))
    positions = (offset + jnp.arange(rows, dtype=jnp.int32)).astype(jnp.float32)
    angles = positions[:, None] * frequency[None, :]
    cos_part = jnp.cos(angles)
    sin_part = jnp.sin(angles)
    return (
        jnp.concatenate([cos_part] * 4, axis=1),
        jnp.concatenate([-sin_part, sin_part] * 2, axis=1),
    )


def body(mesh, hidden_in, pre_gain, query_proj, key_proj, value_proj, out_proj, post_gain):
    rows, depth = hidden_in.shape
    width = query_proj.shape[1]
    n_tp = mesh.shape["tp"]
    group = group_of(mesh, width)
    part = width // group
    s = lax.axis_index("sp")
    t = lax.axis_index("tp")
    c = lax.rem(s, group)
    all_rows = rows * group
    behind = -(-(WIDE * SPAN) // all_rows)
    hid, wk, wv = gather(mesh, group, hidden_in, key_proj, value_proj)
    wq = lax.dynamic_slice_in_dim(query_proj, c * part, part, axis=1)
    cos_part, sin_part = tables(all_rows, (s - c) * rows)
    nat, res = project(
        hid.reshape(all_rows, depth), pre_gain[None, :], wq, wk, wv, cos_part, sin_part
    )
    att, lw = attend(mesh, group, behind, nat, res)
    attended, log_weight = give_back(mesh, group, att, lw)
    partial = jnp.dot(attended, out_proj, preferred_element_type=jnp.float32).astype(jnp.bfloat16)
    partial = partial.reshape(n_tp, rows // n_tp, depth)
    others = swap(mesh, partial)
    own = lax.dynamic_index_in_dim(partial, t, 0, keepdims=False)
    summed = own.astype(jnp.float32) + jnp.sum(others.astype(jnp.float32), axis=0)
    scale = lax.rsqrt(jnp.mean(summed * summed, axis=-1, keepdims=True) + EPS)
    layer_out = (summed * scale * post_gain).astype(jnp.bfloat16)
    return (layer_out, log_weight.reshape(width // HEAD_DIM, rows))


def solution(mesh):
    placed = (P("sp", None), P(), P(None, "tp"), P("sp", "tp"), P("sp", "tp"), P("tp", None), P())
    return jax.shard_map(
        functools.partial(body, mesh),
        mesh=mesh,
        in_specs=placed,
        out_specs=(P(("sp", "tp"), None), P("tp", "sp")),
        check_vma=False,
    )
```
